32 devices in a mesh: fs: 4 (over z), rep: 4 (over y, x), tp: 2 (over core).
Axes of the slice: x: 2, y: 2, z: 4, core: 2. Of those that a mesh axis runs over, the one named last changes fastest.
Arguments:
- normed_in: bfloat16 [16384, 2048], P(('fs', 'rep')), may hold values from -6 to 6
- inner_cot: bfloat16 [16384, 4096], P(('fs', 'rep'), 'tp'), may hold values from -6 to 6
- gated_mid: bfloat16 [16384, 4096], P(('fs', 'rep')), may hold values from -6 to 6
- output_cot: bfloat16 [16384, 2048], P(('fs', 'rep'), 'tp'), may hold values from -6 to 6
- basis_in: bfloat16 [2048, 256], replicated, may hold values from -0.125 to 0.125
- basis_mid: bfloat16 [4096, 256], replicated, may hold values from -0.09375 to 0.09375
- master_in: float32 [2048, 4096], P(('fs', 'rep'), 'tp'), may hold values from -6 to 6
- master_mid: float32 [4096, 2048], P(('fs', 'rep'), 'tp'), may hold values from -6 to 6
- first_in: float32 [256, 4096], P(('fs', 'rep'), 'tp'), may hold values from -160 to 160
- second_in: float32 [256, 4096], P(('fs', 'rep'), 'tp'), may hold values from 163.84 to 29491.2, as said below
- first_mid: float32 [256, 2048], P(('fs', 'rep'), 'tp'), may hold values from -160 to 160
- second_mid: float32 [256, 2048], P(('fs', 'rep'), 'tp'), may hold values from 163.84 to 29491.2, as said below
Outputs:
- step_in: float32 [2048, 4096], P(('fs', 'rep'), 'tp')
- step_mid: float32 [4096, 2048], P(('fs', 'rep'), 'tp')
- moment_in: float32 [256, 4096], P(('fs', 'rep'), 'tp')
- square_in: float32 [256, 4096], P(('fs', 'rep'), 'tp')
- moment_mid: float32 [256, 2048], P(('fs', 'rep'), 'tp')
- square_mid: float32 [256, 2048], P(('fs', 'rep'), 'tp')
- copy_in: bfloat16 [2048, 4096], P('fs', 'tp')
- copy_mid: bfloat16 [4096, 2048], P('fs', 'tp')
The draws below stay inside these ranges and needn't reach their ends.
Inputs may be any that keep to these rules, and one draw needn't show every extreme that they name: `second_in`: positive second moments. `second_mid`: positive second moments.
All inputs are finite; a program needn't handle non-finite values.
Results may differ from the reference program's by a relative error of at most 0.0036.
Values may be sent and summed in bfloat16 or wider, within the bound.
A program may use at most 128 MiB of HBM per device.

```python
import jax
import jax.numpy as jnp
from jax import lax

D = 2048
DI = 4096
RANK = 256
TOK_DEV = 1024
TOKENS = 16384


def rising(key, rows, cols):
    unit = jax.random.uniform(key, (rows, cols), jnp.float32)
    row_pos = jnp.arange(rows, dtype=jnp.float32)[:, None] / rows
    col_pos = jnp.arange(cols, dtype=jnp.float32)[None, :] / cols
    base = jnp.exp(jnp.log(0.01) + unit * (jnp.log(0.2) - jnp.log(0.01)))
    lift = jnp.power(3.0, row_pos) * jnp.power(3.0, col_pos)
    return (TOKENS * base * lift).astype(jnp.float32)


def draw_second_in(key, part):
    return rising(jax.random.fold_in(key, 3), RANK, DI)


def draw_second_mid(key, part):
    return rising(jax.random.fold_in(key, 7), RANK, D)


def levels(own_key, dims, split, least, top_value):
    gain, own = 1.0, jax.random.fold_in(own_key, 6)
    for dim, shards_of in split:
        heights = jnp.exp(jax.random.uniform(jax.random.fold_in(own, dim), (shards_of,), jnp.float32, least / len(split), top_value / len(split)))
        gain = gain * jnp.repeat(heights, dims[dim] // shards_of).reshape([-1 if axis == dim else 1 for axis in range(len(dims))])
    return gain


def centred(own_key, extent, width, bound, split=(), held_as=jnp.bfloat16):
    array = width * jax.random.normal(own_key, extent, jnp.float32)
    if split:
        array = array * levels(own_key, extent, split, -0.22, 0.18)
    return jnp.clip(array, -bound, bound).astype(held_as)


def setup_inputs(seed: int = 0) -> dict:
    keys = jax.random.split(jax.random.key(seed), 13)
    normed_in = centred(keys[0], (TOKENS, D), 1.0, 6.0, ((0, 16),))
    inner_cot = centred(keys[1], (TOKENS, DI), 1.0, 6.0, ((0, 16), (1, 2)))
    gated_mid = centred(keys[2], (TOKENS, DI), 1.0, 6.0, ((0, 16),))
    output_cot = centred(keys[3], (TOKENS, D), 1.0, 6.0, ((0, 16), (1, 2)))
    basis_in = centred(keys[4], (D, RANK), D ** -0.5, 0.125)
    basis_mid = centred(keys[5], (DI, RANK), DI ** -0.5, 0.09375)
    master_in = centred(keys[6], (D, DI), 1.0, 6.0, ((0, 16), (1, 2)), jnp.float32)
    master_mid = centred(keys[7], (DI, D), 1.0, 6.0, ((0, 16), (1, 2)), jnp.float32)
    first_in = centred(keys[8], (RANK, DI), (0.2 * TOKENS ** 0.5), 160.0, ((0, 16), (1, 2)), jnp.float32)
    second_in = draw_second_in(jax.random.fold_in(keys[12], 71), 0)
    first_mid = centred(keys[10], (RANK, D), (0.2 * TOKENS ** 0.5), 160.0, ((0, 16), (1, 2)), jnp.float32)
    second_mid = draw_second_mid(jax.random.fold_in(keys[12], 71), 0)
    return dict(normed_in=normed_in, inner_cot=inner_cot, gated_mid=gated_mid, output_cot=output_cot, basis_in=basis_in, basis_mid=basis_mid, master_in=master_in, master_mid=master_mid, first_in=first_in, second_in=second_in, first_mid=first_mid, second_mid=second_mid)


beta_one = 0.9
beta_two = 0.95
rate_scale = 0.5

def projected(inputs, cotangent, basis):
    groups = inputs.shape[0] // TOK_DEV
    stacked_in = inputs.reshape(groups, TOK_DEV, inputs.shape[1])
    stacked_cot = cotangent.reshape(groups, TOK_DEV, cotangent.shape[1])

    def accumulate(total, pair):
        rows_in, rows_cot = pair
        low_rank = jnp.dot(rows_in, basis, preferred_element_type=jnp.float32)
        term = lax.dot_general(low_rank, rows_cot.astype(jnp.float32), (((0,), (0,)), ((), ())), precision=lax.Precision.HIGHEST)
        return (total + term, None)
    start = jnp.zeros((basis.shape[1], cotangent.shape[1]), jnp.float32)
    total, _ = lax.scan(accumulate, start, (stacked_in, stacked_cot))
    return total

def adjust(first, second, proj, basis, master):
    moment = beta_one * first + (1.0 - beta_one) * proj
    square = beta_two * second + (1.0 - beta_two) * proj * proj
    direction = moment / jnp.sqrt(square)
    scale = rate_scale * lax.rsqrt(jnp.mean(direction * direction) + 1e-06)
    update = jnp.dot(basis.astype(jnp.float32), direction, precision=lax.Precision.HIGHEST)
    step = scale * update
    fresh = (master - step).astype(jnp.bfloat16)
    return (step, moment, square, fresh)

def reference(normed_in, inner_cot, gated_mid, output_cot, basis_in, basis_mid, master_in, master_mid, first_in, second_in, first_mid, second_mid):
    proj_in = projected(normed_in, inner_cot, basis_in)
    proj_mid = projected(gated_mid, output_cot, basis_mid)
    step_in, moment_in, square_in, copy_in = adjust(first_in, second_in, proj_in, basis_in, master_in)
    step_mid, moment_mid, square_mid, copy_mid = adjust(first_mid, second_mid, proj_mid, basis_mid, master_mid)
    return (step_in, step_mid, moment_in, square_in, moment_mid, square_mid, copy_in, copy_mid)
```

```python
import functools

import jax
import jax.numpy as jnp
from jax import lax
from jax.experimental import pallas as pl
from jax.experimental.pallas import tpu as pltpu
from jax.sharding import PartitionSpec as P

beta_one = 0.9
beta_two = 0.95
rate_scale = 0.5

MESH = pl.DeviceIdType.MESH


def remote(src, dst, send, recv, where):
    return pltpu.make_async_remote_copy(
        src_ref=src, dst_ref=dst, send_sem=send, recv_sem=recv, device_id=where, device_id_type=MESH
    )


def exchange(
    sizes,
    low_in, low_mid, cot_in, cot_mid, master_in, master_mid,
    first_in, second_in, first_mid, second_mid,
    ways, weights_in, weights_mid, moment_in, square_in, moment_mid, square_mid, totals,
    cots, whole, own, part, zland, spread, xland, sums,
    cot_sem, zsend, zrecv, xsend, xrecv, msend, mrecv, mlocal, gzs, gxs, gys, gdiag, grecv, tsend, trecv,
):
    F, R, T, rows, width, n_in, n_mid = sizes
    nt = n_in + n_mid
    rank = F * R * rows
    f, r, t = lax.axis_index("fs"), lax.axis_index("rep"), lax.axis_index("tp")
    cols_in = n_in * width

    def cot_copy(c, source, base):
        return pltpu.make_async_copy(
            source.at[:, pl.ds(pl.multiple_of((c - base) * width, width), width)], cots.at[c], cot_sem.at[c]
        )

    for c in range(nt):
        (cot_copy(c, cot_in, 0) if c < n_in else cot_copy(c, cot_mid, n_in)).start()
    local_in = pltpu.make_async_copy(master_in, weights_in.at[r], mlocal.at[0])
    local_mid = pltpu.make_async_copy(master_mid, weights_mid.at[r], mlocal.at[1])
    local_in.start()
    local_mid.start()

    barrier = pltpu.get_barrier_semaphore()
    for k in range(1, F):
        pl.semaphore_signal(barrier, inc=1, device_id={"fs": lax.rem(f + k, F)}, device_id_type=MESH)
    for k in range(1, R):
        pl.semaphore_signal(barrier, inc=1, device_id={"rep": lax.rem(r + k, R)}, device_id_type=MESH)
    for k in range(1, T):
        pl.semaphore_signal(barrier, inc=1, device_id={"tp": lax.rem(t + k, T)}, device_id_type=MESH)
    pl.semaphore_wait(barrier, F + R + T - 3)

    half = R // 2
    high, low = r // half, lax.rem(r, half)
    near = high * half + (half - 1 - low)
    far = (1 - high) * half + low
    cross = (1 - high) * half + (half - 1 - low)

    def m_copy(which, source, peer, slot, index):
        array = weights_in if which == 0 else weights_mid
        return remote(source, array.at[slot], msend.at[index], mrecv.at[index], {"rep": peer})

    m_sends = [
        m_copy(0, master_in, near, r, 0),
        m_copy(1, master_mid, far, r, 1),
        m_copy(1, master_mid, near, r, 2),
        m_copy(0, master_in, far, r, 3),
    ]
    m_recvs = [
        m_copy(0, master_in, near, near, 0),
        m_copy(1, master_mid, far, far, 1),
        m_copy(1, master_mid, near, near, 2),
        m_copy(0, master_in, far, far, 3),
        m_copy(0, master_in, far, cross, 4),
        m_copy(1, master_mid, near, cross, 5),
    ]
    for copy in m_sends:
        copy.start()

    def z_copy(c, peer, slot, to):
        return remote(part.at[c, peer], zland.at[c, slot], zsend.at[c, peer], zrecv.at[c, slot], {"fs": to})

    def contract(low_ref, source, base, c):
        cot_copy(c, source, base).wait()
        both = jnp.dot(low_ref[...], cots[c], preferred_element_type=jnp.float32)
        joint = (both[:rank] + both[rank:]).reshape(F, R * rows, width)
        whole[...] = joint
        part[c] = joint.astype(jnp.bfloat16)
        own[c] = whole[f]
        for k in range(1, F):
            peer = lax.rem(f + k, F)
            z_copy(c, peer, f, peer).start()

    @pl.loop(0, n_in)
    def _(c):
        contract(low_in, cot_in, 0, c)

    @pl.loop(n_in, nt)
    def _(c):
        contract(low_mid, cot_mid, n_in, c)

    def x_copy(c, peer, slot):
        return remote(spread.at[c, peer], xland.at[c, slot], xsend.at[c, peer], xrecv.at[c, slot], {"rep": peer})

    def gather_sum(c):
        total = own[c]
        for k in range(1, F):
            peer = lax.rem(f + k, F)
            z_copy(c, peer, peer, peer).wait_recv()
            total = total + zland[c, peer].astype(jnp.float32)
        for k in range(R):
            spread[c, k] = total[k * rows : (k + 1) * rows]
        for k in range(1, R):
            peer = lax.rem(r + k, R)
            x_copy(c, peer, r).start()

    def update(c):
        proj = spread[c, r]
        for k in range(1, R):
            peer = lax.rem(r + k, R)
            x_copy(c, peer, peer).wait_recv()
            proj = proj + xland[c, peer]
        if c < n_in:
            span = slice(c * width, (c + 1) * width)
            first, second, moment_ref, square_ref = first_in, second_in, moment_in, square_in
        else:
            span = slice((c - n_in) * width, (c - n_in + 1) * width)
            first, second, moment_ref, square_ref = first_mid, second_mid, moment_mid, square_mid
        moment = beta_one * first[:, span] + (1.0 - beta_one) * proj
        square = beta_two * second[:, span] + (1.0 - beta_two) * proj * proj
        moment_ref[:, span] = moment
        square_ref[:, span] = square
        ways[f, r, :, c * width : (c + 1) * width] = (moment / jnp.sqrt(square)).astype(jnp.bfloat16)

    relays = [
        m_copy(0, weights_in.at[near], far, near, 4),
        m_copy(1, weights_mid.at[far], near, far, 5),
    ]
    relay_at = nt // 2
    for c in range(nt):
        gather_sum(c)
        if c == relay_at:
            m_recvs[0].wait_recv()
            relays[0].start()
            m_recvs[1].wait_recv()
            relays[1].start()
        if c > 0:
            update(c - 1)
    update(nt - 1)

    def g_copy(i, j, send, where):
        return remote(ways.at[i, j], ways.at[i, j], send, grecv.at[i, j], where)

    for k in range(1, F):
        peer = lax.rem(f + k, F)
        g_copy(f, r, gzs.at[k], {"fs": peer}).start()

    def onward(k):
        i = lax.rem(f + k, F)
        if k > 0:
            g_copy(i, r, gzs.at[k], {"fs": i}).wait_recv()
        g_copy(i, r, gxs.at[k], {"rep": near}).start()
        g_copy(i, r, gys.at[k], {"rep": far}).start()

    def relay(k):
        i = lax.rem(f + k, F)
        if k % 2 == 0:
            g_copy(i, near, gdiag.at[k], {"rep": far}).wait_recv()
            g_copy(i, near, gdiag.at[k], {"rep": far}).start()
        else:
            g_copy(i, far, gdiag.at[k], {"rep": near}).wait_recv()
            g_copy(i, far, gdiag.at[k], {"rep": near}).start()

    onward(0)
    for k in range(1, F):
        onward(k)
        relay(k - 1)
    relay(F - 1)
    for k in range(F):
        i = lax.rem(f + k, F)
        g_copy(i, far if k % 2 == 0 else near, gdiag.at[k], {"rep": far}).wait_recv()
        g_copy(i, cross, gdiag.at[k], {"rep": far}).wait_recv()

    square_sum = jnp.zeros((rows, nt * width), jnp.float32)

    def add_piece(i, acc):
        for j in range(R):
            piece = ways[i, j].astype(jnp.float32)
            acc = acc + piece * piece
        return acc

    square_sum = lax.fori_loop(0, F, add_piece, square_sum)
    sums[t, 0] = jnp.full(sums.shape[2:], jnp.sum(square_sum[:, :cols_in]), jnp.float32)
    sums[t, 1] = jnp.full(sums.shape[2:], jnp.sum(square_sum[:, cols_in:]), jnp.float32)

    def t_copy(peer, slot):
        return remote(sums.at[slot], sums.at[slot], tsend.at[peer], trecv.at[slot], {"tp": peer})

    for k in range(1, T):
        t_copy(lax.rem(t + k, T), t).start()

    for index in range(2, 6):
        m_recvs[index].wait_recv()
    for copy in m_sends + relays:
        copy.wait_send()
    local_in.wait()
    local_mid.wait()
    for k in range(1, F):
        peer = lax.rem(f + k, F)
        for c in range(nt):
            z_copy(c, peer, f, peer).wait_send()
        g_copy(f, r, gzs.at[k], {"fs": peer}).wait_send()
    for k in range(1, R):
        peer = lax.rem(r + k, R)
        for c in range(nt):
            x_copy(c, peer, r).wait_send()
    for k in range(F):
        i = lax.rem(f + k, F)
        g_copy(i, r, gxs.at[k], {"rep": near}).wait_send()
        g_copy(i, r, gys.at[k], {"rep": far}).wait_send()
        g_copy(i, near, gdiag.at[k], {"rep": far}).wait_send()
    for k in range(1, T):
        peer = lax.rem(t + k, T)
        t_copy(peer, peer).wait_recv()
        t_copy(peer, t).wait_send()
    total = sums[0]
    for k in range(1, T):
        total = total + sums[k]
    totals[...] = total


def body(
    shape,
    normed_in, inner_cot, gated_mid, output_cot, basis_in, basis_mid,
    master_in, master_mid, first_in, second_in, first_mid, second_mid,
):
    F, R, T = shape
    rank = basis_in.shape[1]
    rows, cols_in = first_in.shape
    cols_mid = first_mid.shape[1]
    tokens = normed_in.shape[0]
    width = 512
    n_in, n_mid = cols_in // width, cols_mid // width
    nt = n_in + n_mid

    def split(basis, inputs):
        lowered = lax.dot_general(basis, inputs, (((0,), (1,)), ((), ())), preferred_element_type=jnp.float32)
        upper = lowered.astype(jnp.bfloat16)
        lower = (lowered - upper.astype(jnp.float32)).astype(jnp.bfloat16)
        return jnp.concatenate([upper, lower], axis=0)

    low_in = split(basis_in, normed_in)
    low_mid = split(basis_mid, gated_mid)
    rough_in = master_in.astype(jnp.bfloat16)
    rough_mid = master_mid.astype(jnp.bfloat16)

    vmem = pl.BlockSpec(memory_space=pltpu.VMEM)
    anywhere = pl.BlockSpec(memory_space=pl.ANY)
    dma = pltpu.SemaphoreType.DMA
    f32, bf16 = jnp.float32, jnp.bfloat16
    small = jax.ShapeDtypeStruct
    ways, weights_in, weights_mid, moment_in, square_in, moment_mid, square_mid, totals = pl.pallas_call(
        functools.partial(exchange, (F, R, T, rows, width, n_in, n_mid)),
        out_shape=(
            small((F, R, rows, nt * width), bf16),
            small((R,) + master_in.shape, bf16),
            small((R,) + master_mid.shape, bf16),
            small(first_in.shape, f32),
            small(first_in.shape, f32),
            small(first_mid.shape, f32),
            small(first_mid.shape, f32),
            small((2, 8, 128), f32),
        ),
        in_specs=[vmem, vmem, anywhere, anywhere, vmem, vmem, vmem, vmem, vmem, vmem],
        out_specs=(vmem, anywhere, anywhere, vmem, vmem, vmem, vmem, vmem),
        scratch_shapes=[
            pltpu.VMEM((nt, tokens, width), bf16),
            pltpu.VMEM((F, R * rows, width), f32),
            pltpu.VMEM((nt, R * rows, width), f32),
            pltpu.VMEM((nt, F, R * rows, width), bf16),
            pltpu.VMEM((nt, F, R * rows, width), bf16),
            pltpu.VMEM((nt, R, rows, width), f32),
            pltpu.VMEM((nt, R, rows, width), f32),
            pltpu.VMEM((T, 2, 8, 128), f32),
            dma((nt,)),
            dma((nt, F)),
            dma((nt, F)),
            dma((nt, R)),
            dma((nt, R)),
            dma((6,)),
            dma((6,)),
            dma((2,)),
            dma((F,)),
            dma((F,)),
            dma((F,)),
            dma((F,)),
            dma((F, R)),
            dma((T,)),
            dma((T,)),
        ],
        compiler_params=pltpu.CompilerParams(
            collective_id=0, has_side_effects=True, vmem_limit_bytes=48 * 1024 * 1024
        ),
    )(
        low_in, low_mid, inner_cot, output_cot, rough_in, rough_mid,
        first_in, second_in, first_mid, second_mid,
    )

    f, slot = lax.axis_index("fs"), lax.axis_index(("fs", "rep"))
    flat = ways.reshape(rank, nt * width)

    def finish(total, columns, basis, master, weights, way):
        scale = rate_scale * lax.rsqrt(total / (rank * columns * T) + 1e-06)
        count = master.shape[0]
        mine = lax.dynamic_slice_in_dim(basis, slot * count, count, 0)
        group = lax.dynamic_slice_in_dim(basis, f * count * R, count * R, 0)
        step = scale * jnp.dot(mine, way, preferred_element_type=f32)
        course = scale * jnp.dot(group, way, preferred_element_type=f32)
        copy = (weights.reshape(count * R, columns).astype(f32) - course).astype(bf16)
        return step, copy

    step_in, copy_in = finish(totals[0, 0, 0], cols_in, basis_in, master_in, weights_in, flat[:, :cols_in])
    step_mid, copy_mid = finish(totals[1, 0, 0], cols_mid, basis_mid, master_mid, weights_mid, flat[:, cols_in:])
    return (step_in, step_mid, moment_in, square_in, moment_mid, square_mid, copy_in, copy_mid)


def solution(mesh):
    both = P(("fs", "rep"), "tp")
    in_specs = (
        P(("fs", "rep"), None), both, P(("fs", "rep"), None), both, P(), P(),
        both, both, both, both, both, both,
    )
    out_specs = (both, both, both, both, both, both, P("fs", "tp"), P("fs", "tp"))
    shape = (mesh.shape["fs"], mesh.shape["rep"], mesh.shape["tp"])
    return jax.shard_map(
        functools.partial(body, shape), mesh=mesh, in_specs=in_specs, out_specs=out_specs, check_vma=False
    )
```

```python
import functools

import jax
import jax.numpy as jnp
from jax import lax
from jax.experimental import pallas as pl
from jax.experimental.pallas import tpu as pltpu
from jax.sharding import PartitionSpec as P

beta_one = 0.9
beta_two = 0.95
rate_scale = 0.5

MESH = pl.DeviceIdType.MESH


def remote(src, dst, send, recv, where):
    return pltpu.make_async_remote_copy(
        src_ref=src, dst_ref=dst, send_sem=send, recv_sem=recv, device_id=where, device_id_type=MESH
    )


def exchange(
    sizes,
    normed, gated, basis_in, basis_mid, cot_in, cot_mid, exact_in, exact_mid,
    first_in, second_in, first_mid, second_mid,
    ways, weights_in, weights_mid, moment_in, square_in, moment_mid, square_mid, totals,
    full_in, full_mid, master_in, master_mid, tall_in, tall_mid, left_in, left_mid, low_in, low_mid,
    cots, whole, own, part, zland, spread, xland, sums,
    load_sem, left_sem, cot_sem, zsend, zrecv, xsend, xrecv, msend, mrecv, mlocal, gzs, gxs, gys, gdiag, grecv, tsend, trecv,
):
    F, R, T, rows, width, n_in, n_mid = sizes
    nt = n_in + n_mid
    rank = F * R * rows
    f, r, t = lax.axis_index("fs"), lax.axis_index("rep"), lax.axis_index("tp")
    cols_in = n_in * width

    def cot_copy(c, source, base):
        return pltpu.make_async_copy(
            source.at[:, pl.ds(pl.multiple_of((c - base) * width, width), width)], cots.at[c], cot_sem.at[c]
        )

    steps = left_sem.shape[1]
    deep = normed.shape[0] // steps

    def left_copy(which, k):
        source, target = ((normed, left_in), (gated, left_mid))[which]
        span = pl.ds(pl.multiple_of(k * deep, deep), deep)
        return pltpu.make_async_copy(source.at[span], target.at[span], left_sem.at[which, k])

    loads = [
        pltpu.make_async_copy(exact_in, full_in, load_sem.at[0]),
        pltpu.make_async_copy(exact_mid, full_mid, load_sem.at[1]),
        pltpu.make_async_copy(basis_in, tall_in, load_sem.at[2]),
        pltpu.make_async_copy(basis_mid, tall_mid, load_sem.at[3]),
    ]
    for load in loads[:3]:
        load.start()
    for k in range(steps):
        left_copy(0, k).start()
    for c in range(n_in):
        cot_copy(c, cot_in, 0).start()
    loads[3].start()
    for k in range(steps):
        left_copy(1, k).start()
    for c in range(n_in, nt):
        cot_copy(c, cot_mid, n_in).start()
    local_in = pltpu.make_async_copy(master_in, weights_in.at[r], mlocal.at[0])
    local_mid = pltpu.make_async_copy(master_mid, weights_mid.at[r], mlocal.at[1])

    barrier = pltpu.get_barrier_semaphore()
    for k in range(1, F):
        pl.semaphore_signal(barrier, inc=1, device_id={"fs": lax.rem(f + k, F)}, device_id_type=MESH)
    for k in range(1, R):
        pl.semaphore_signal(barrier, inc=1, device_id={"rep": lax.rem(r + k, R)}, device_id_type=MESH)
    for k in range(1, T):
        pl.semaphore_signal(barrier, inc=1, device_id={"tp": lax.rem(t + k, T)}, device_id_type=MESH)
    loads[0].wait()
    master_in[...] = full_in[...].astype(jnp.bfloat16)
    loads[1].wait()
    master_mid[...] = full_mid[...].astype(jnp.bfloat16)
    pl.semaphore_wait(barrier, F + R + T - 3)

    half = R // 2
    high, low = r // half, lax.rem(r, half)
    near = high * half + (half - 1 - low)
    far = (1 - high) * half + low
    cross = (1 - high) * half + (half - 1 - low)

    def m_copy(which, source, peer, slot, index):
        array = weights_in if which == 0 else weights_mid
        return remote(source, array.at[slot], msend.at[index], mrecv.at[index], {"rep": peer})

    m_sends = [
        m_copy(0, master_in, near, r, 0),
        m_copy(1, master_mid, far, r, 1),
        m_copy(1, master_mid, near, r, 2),
        m_copy(0, master_in, far, r, 3),
    ]
    m_recvs = [
        m_copy(0, master_in, near, near, 0),
        m_copy(1, master_mid, far, far, 1),
        m_copy(1, master_mid, near, near, 2),
        m_copy(0, master_in, far, far, 3),
        m_copy(0, master_in, far, cross, 4),
        m_copy(1, master_mid, near, cross, 5),
    ]
    for copy in m_sends:
        copy.start()
    local_in.start()
    local_mid.start()

    def lower(which, tall, low_ref):
        loads[2 + which].wait()

        @pl.loop(0, steps)
        def _(k):
            left_copy(which, k).wait()
            span = pl.ds(pl.multiple_of(k * deep, deep), deep)
            left = (left_in, left_mid)[which]
            low = jnp.dot(left[span, :], tall[...], preferred_element_type=jnp.float32).T
            upper = low.astype(jnp.bfloat16)
            low_ref[:rank, span] = upper
            low_ref[rank:, span] = (low - upper.astype(jnp.float32)).astype(jnp.bfloat16)

    def z_copy(c, peer, slot, to):
        return remote(part.at[c, peer], zland.at[c, slot], zsend.at[c, peer], zrecv.at[c, slot], {"fs": to})

    def contract(low_ref, source, base, c):
        cot_copy(c, source, base).wait()
        both = jnp.dot(low_ref[...], cots[c], preferred_element_type=jnp.float32)
        joint = (both[:rank] + both[rank:]).reshape(F, R * rows, width)
        whole[...] = joint
        part[c] = joint.astype(jnp.bfloat16)
        own[c] = whole[f]
        for k in range(1, F):
            peer = lax.rem(f + k, F)
            z_copy(c, peer, f, peer).start()

    lower(0, tall_in, low_in)

    @pl.loop(0, n_in)
    def _(c):
        contract(low_in, cot_in, 0, c)

    lower(1, tall_mid, low_mid)

    @pl.loop(n_in, nt)
    def _(c):
        contract(low_mid, cot_mid, n_in, c)

    def x_copy(c, peer, slot):
        return remote(spread.at[c, peer], xland.at[c, slot], xsend.at[c, peer], xrecv.at[c, slot], {"rep": peer})

    def gather_sum(c):
        total = own[c]
        for k in range(1, F):
            peer = lax.rem(f + k, F)
            z_copy(c, peer, peer, peer).wait_recv()
            total = total + zland[c, peer].astype(jnp.float32)
        for k in range(R):
            spread[c, k] = total[k * rows : (k + 1) * rows]
        for k in range(1, R):
            peer = lax.rem(r + k, R)
            x_copy(c, peer, r).start()

    def update(c):
        proj = spread[c, r]
        for k in range(1, R):
            peer = lax.rem(r + k, R)
            x_copy(c, peer, peer).wait_recv()
            proj = proj + xland[c, peer]
        if c < n_in:
            span = slice(c * width, (c + 1) * width)
            first, second, moment_ref, square_ref = first_in, second_in, moment_in, square_in
        else:
            span = slice((c - n_in) * width, (c - n_in + 1) * width)
            first, second, moment_ref, square_ref = first_mid, second_mid, moment_mid, square_mid
        moment = beta_one * first[:, span] + (1.0 - beta_one) * proj
        square = beta_two * second[:, span] + (1.0 - beta_two) * proj * proj
        moment_ref[:, span] = moment
        square_ref[:, span] = square
        ways[f, r, :, c * width : (c + 1) * width] = (moment / jnp.sqrt(square)).astype(jnp.bfloat16)

    relays = [
        m_copy(0, weights_in.at[near], far, near, 4),
        m_copy(1, weights_mid.at[far], near, far, 5),
    ]
    relay_at = nt // 2
    for c in range(nt):
        gather_sum(c)
        if c == relay_at:
            m_recvs[0].wait_recv()
            relays[0].start()
            m_recvs[1].wait_recv()
            relays[1].start()
        if c > 0:
            update(c - 1)
    update(nt - 1)

    def g_copy(i, j, send, where):
        return remote(ways.at[i, j], ways.at[i, j], send, grecv.at[i, j], where)

    for k in range(1, F):
        peer = lax.rem(f + k, F)
        g_copy(f, r, gzs.at[k], {"fs": peer}).start()

    def onward(k):
        i = lax.rem(f + k, F)
        if k > 0:
            g_copy(i, r, gzs.at[k], {"fs": i}).wait_recv()
        g_copy(i, r, gxs.at[k], {"rep": near}).start()
        g_copy(i, r, gys.at[k], {"rep": far}).start()

    def relay(k):
        i = lax.rem(f + k, F)
        if k % 2 == 0:
            g_copy(i, near, gdiag.at[k], {"rep": far}).wait_recv()
            g_copy(i, near, gdiag.at[k], {"rep": far}).start()
        else:
            g_copy(i, far, gdiag.at[k], {"rep": near}).wait_recv()
            g_copy(i, far, gdiag.at[k], {"rep": near}).start()

    onward(0)
    for k in range(1, F):
        onward(k)
        relay(k - 1)
    relay(F - 1)
    for k in range(F):
        i = lax.rem(f + k, F)
        g_copy(i, far if k % 2 == 0 else near, gdiag.at[k], {"rep": far}).wait_recv()
        g_copy(i, cross, gdiag.at[k], {"rep": far}).wait_recv()

    square_sum = jnp.zeros((rows, nt * width), jnp.float32)

    def add_piece(i, acc):
        for j in range(R):
            piece = ways[i, j].astype(jnp.float32)
            acc = acc + piece * piece
        return acc

    square_sum = lax.fori_loop(0, F, add_piece, square_sum)
    sums[t, 0] = jnp.full(sums.shape[2:], jnp.sum(square_sum[:, :cols_in]), jnp.float32)
    sums[t, 1] = jnp.full(sums.shape[2:], jnp.sum(square_sum[:, cols_in:]), jnp.float32)

    def t_copy(peer, slot):
        return remote(sums.at[slot], sums.at[slot], tsend.at[peer], trecv.at[slot], {"tp": peer})

    for k in range(1, T):
        t_copy(lax.rem(t + k, T), t).start()

    for index in range(2, 6):
        m_recvs[index].wait_recv()
    for copy in m_sends + relays:
        copy.wait_send()
    local_in.wait()
    local_mid.wait()
    for k in range(1, F):
        peer = lax.rem(f + k, F)
        for c in range(nt):
            z_copy(c, peer, f, peer).wait_send()
        g_copy(f, r, gzs.at[k], {"fs": peer}).wait_send()
    for k in range(1, R):
        peer = lax.rem(r + k, R)
        for c in range(nt):
            x_copy(c, peer, r).wait_send()
    for k in range(F):
        i = lax.rem(f + k, F)
        g_copy(i, r, gxs.at[k], {"rep": near}).wait_send()
        g_copy(i, r, gys.at[k], {"rep": far}).wait_send()
        g_copy(i, near, gdiag.at[k], {"rep": far}).wait_send()
    for k in range(1, T):
        peer = lax.rem(t + k, T)
        t_copy(peer, peer).wait_recv()
        t_copy(peer, t).wait_send()
    total = sums[0]
    for k in range(1, T):
        total = total + sums[k]
    totals[...] = total


def body(
    shape,
    normed_in, inner_cot, gated_mid, output_cot, basis_in, basis_mid,
    master_in, master_mid, first_in, second_in, first_mid, second_mid,
):
    F, R, T = shape
    rank = basis_in.shape[1]
    rows, cols_in = first_in.shape
    cols_mid = first_mid.shape[1]
    tokens = normed_in.shape[0]
    width = 512
    n_in, n_mid = cols_in // width, cols_mid // width
    nt = n_in + n_mid

    vmem = pl.BlockSpec(memory_space=pltpu.VMEM)
    anywhere = pl.BlockSpec(memory_space=pl.ANY)
    dma = pltpu.SemaphoreType.DMA
    f32, bf16 = jnp.float32, jnp.bfloat16
    small = jax.ShapeDtypeStruct
    ways, weights_in, weights_mid, moment_in, square_in, moment_mid, square_mid, totals = pl.pallas_call(
        functools.partial(exchange, (F, R, T, rows, width, n_in, n_mid)),
        out_shape=(
            small((F, R, rows, nt * width), bf16),
            small((R,) + master_in.shape, bf16),
            small((R,) + master_mid.shape, bf16),
            small(first_in.shape, f32),
            small(first_in.shape, f32),
            small(first_mid.shape, f32),
            small(first_mid.shape, f32),
            small((2, 8, 128), f32),
        ),
        in_specs=[anywhere] * 8 + [vmem] * 4,
        out_specs=(vmem, anywhere, anywhere, vmem, vmem, vmem, vmem, vmem),
        scratch_shapes=[
            pltpu.VMEM(master_in.shape, f32),
            pltpu.VMEM(master_mid.shape, f32),
            pltpu.VMEM(master_in.shape, bf16),
            pltpu.VMEM(master_mid.shape, bf16),
            pltpu.VMEM(basis_in.shape, bf16),
            pltpu.VMEM(basis_mid.shape, bf16),
            pltpu.VMEM(normed_in.shape, bf16),
            pltpu.VMEM(gated_mid.shape, bf16),
            pltpu.VMEM((2 * rank, tokens), bf16),
            pltpu.VMEM((2 * rank, tokens), bf16),
            pltpu.VMEM((nt, tokens, width), bf16),
            pltpu.VMEM((F, R * rows, width), f32),
            pltpu.VMEM((nt, R * rows, width), f32),
            pltpu.VMEM((nt, F, R * rows, width), bf16),
            pltpu.VMEM((nt, F, R * rows, width), bf16),
            pltpu.VMEM((nt, R, rows, width), f32),
            pltpu.VMEM((nt, R, rows, width), f32),
            pltpu.VMEM((T, 2, 8, 128), f32),
            dma((4,)),
            dma((2, tokens // 512)),
            dma((nt,)),
            dma((nt, F)),
            dma((nt, F)),
            dma((nt, R)),
            dma((nt, R)),
            dma((6,)),
            dma((6,)),
            dma((2,)),
            dma((F,)),
            dma((F,)),
            dma((F,)),
            dma((F,)),
            dma((F, R)),
            dma((T,)),
            dma((T,)),
        ],
        compiler_params=pltpu.CompilerParams(
            collective_id=0, has_side_effects=True, vmem_limit_bytes=56 * 1024 * 1024
        ),
    )(
        normed_in, gated_mid, basis_in, basis_mid, inner_cot, output_cot, master_in, master_mid,
        first_in, second_in, first_mid, second_mid,
    )

    where = jnp.stack([lax.axis_index("fs"), lax.axis_index("rep")]).astype(jnp.int32)
    tall_in, tall_mid = master_in.shape[0], master_mid.shape[0]

    def block(shape, turn):
        return pl.BlockSpec(shape, turn)

    def turned(j, at):
        return lax.rem(at[1] + j, R)

    def still(shape):
        return pl.BlockSpec(shape, lambda j, at: (0,) * len(shape))

    small_specs = [still(x.shape) for x in (moment_in, square_in, moment_mid, square_mid)]
    results = pl.pallas_call(
        functools.partial(finish, (rank * cols_in * T, rank * cols_mid * T, cols_in)),
        grid_spec=pltpu.PrefetchScalarGridSpec(
            num_scalar_prefetch=1,
            grid=(R,),
            in_specs=[
                still((2, 8, 128)),
                still((rank, nt * width)),
                block((tall_in, rank), lambda j, at: (at[0] * R + turned(j, at), 0)),
                block((tall_mid, rank), lambda j, at: (at[0] * R + turned(j, at), 0)),
                block((1, tall_in, cols_in), lambda j, at: (turned(j, at), 0, 0)),
                block((1, tall_mid, cols_mid), lambda j, at: (turned(j, at), 0, 0)),
                *small_specs,
            ],
            out_specs=[
                anywhere,
                anywhere,
                *small_specs,
                block((tall_in, cols_in), lambda j, at: (turned(j, at), 0)),
                block((tall_mid, cols_mid), lambda j, at: (turned(j, at), 0)),
            ],
            scratch_shapes=[
                pltpu.VMEM(master_in.shape, f32),
                pltpu.VMEM(master_mid.shape, f32),
                dma((2,)),
            ],
        ),
        out_shape=[
            small(master_in.shape, f32),
            small(master_mid.shape, f32),
            small(first_in.shape, f32),
            small(first_in.shape, f32),
            small(first_mid.shape, f32),
            small(first_mid.shape, f32),
            small((R * tall_in, cols_in), bf16),
            small((R * tall_mid, cols_mid), bf16),
        ],
        compiler_params=pltpu.CompilerParams(vmem_limit_bytes=56 * 1024 * 1024),
    )(
        where, totals, ways.reshape(rank, nt * width), basis_in, basis_mid, weights_in, weights_mid,
        moment_in, square_in, moment_mid, square_mid,
    )
    return tuple(results)


def finish(
    counts, at, totals, way, basis_in, basis_mid, weights_in, weights_mid, *rest
):
    small_in, (step_in, step_mid), small_out = rest[:4], rest[4:6], rest[6:10]
    copy_in, copy_mid, held_in, held_mid, sems = rest[10:]
    turn = pl.program_id(0)
    out_in = pltpu.make_async_copy(held_in, step_in, sems.at[0])
    out_mid = pltpu.make_async_copy(held_mid, step_mid, sems.at[1])
    sides = (
        (0, counts[0], basis_in, weights_in, copy_in, held_in, out_in, slice(0, counts[2])),
        (1, counts[1], basis_mid, weights_mid, copy_mid, held_mid, out_mid, slice(counts[2], None)),
    )
    for side, count, basis, weights, copy, held, out, span in sides:
        scale = rate_scale * lax.rsqrt(totals[side, 0:1, 0:1] / count + 1e-06)
        step = scale * jnp.dot(basis[...], way[:, span], preferred_element_type=jnp.float32)
        copy[...] = (weights[0].astype(jnp.float32) - step).astype(jnp.bfloat16)

        @pl.when(turn == 0)
        def _():
            held[...] = step
            out.start()

    @pl.when(turn == 0)
    def _():
        for source, target in zip(small_in, small_out):
            target[...] = source[...]

    @pl.when(turn == pl.num_programs(0) - 1)
    def _():
        out_in.wait()
        out_mid.wait()


def solution(mesh):
    both = P(("fs", "rep"), "tp")
    in_specs = (
        P(("fs", "rep"), None), both, P(("fs", "rep"), None), both, P(), P(),
        both, both, both, both, both, both,
    )
    out_specs = (both, both, both, both, both, both, P("fs", "tp"), P("fs", "tp"))
    shape = (mesh.shape["fs"], mesh.shape["rep"], mesh.shape["tp"])
    return jax.shard_map(
        functools.partial(body, shape), mesh=mesh, in_specs=in_specs, out_specs=out_specs, check_vma=False
    )
```
